32 devices in a mesh: fs: 8 (over z, y), tp: 4 (over x, core).
Axes of the slice: x: 2, y: 2, z: 4, core: 2. Of those that a mesh axis runs over, the one named last changes fastest.
Arguments:
- weights_in: float32 [2, 2048, 5632], P(None, 'fs', 'tp'), may hold values from -6 to 6
- weights_mix: float32 [2048, 2048], P('fs', 'tp'), may hold values from -6 to 6
- momentum_in: float32 [2, 2048, 5632], P(None, 'fs', 'tp'), may hold values from -5 to 5
- momentum_mix: float32 [2048, 2048], P('fs', 'tp'), may hold values from -5 to 5
- grads_in: float32 [2, 2048, 5632], P(None, 'fs', 'tp'), may hold values from -5 to 5
- grads_mix: float32 [2048, 2048], P('fs', 'tp'), may hold values from -5 to 5
Outputs:
- momentum_in_next: float32 [2, 2048, 5632], P(None, 'fs', 'tp')
- momentum_mix_next: float32 [2048, 2048], P('fs', 'tp')
- weights_in_next: float32 [2, 2048, 5632], P(None, 'fs', 'tp')
- weights_mix_next: float32 [2048, 2048], P('fs', 'tp')
- update_in: float32 [2, 2048, 5632], P(None, 'fs', 'tp')
- update_mix: float32 [2048, 2048], P('fs', 'tp')
The draws below stay inside these ranges and needn't reach their ends.
All inputs are finite; a program needn't handle non-finite values.
Results may differ from the reference program's by a relative error of at most 0.0003.
Values sent between devices are 32-bit elements; how exact they have to be, the bound alone decides.
A program may use at most 128 MiB of HBM per device.

```python
import math
import jax
import jax.numpy as jnp
from jax import lax

D = 2048
FF = 5632
ITERS = 3


def unit_field(key, shape):
    return jnp.clip(jax.random.normal(key, shape, jnp.float32), -5.0, 5.0)


def draw_momentum_in(key, part):
    return unit_field(jax.random.fold_in(key, 11), (2, D, FF))


def draw_momentum_mix(key, part):
    return unit_field(jax.random.fold_in(key, 12), (D, D))


def draw_grads_in(key, part):
    return unit_field(jax.random.fold_in(key, 13), (2, D, FF))


def draw_grads_mix(key, part):
    return unit_field(jax.random.fold_in(key, 14), (D, D))


def steps_of(key, dims, cuts, smallest, top_value):
    def one(position, parts):
        draws = jax.random.uniform(jax.random.fold_in(jax.random.fold_in(key, 6), position), (parts,), jnp.float32, smallest / len(cuts), top_value / len(cuts))
        return jnp.repeat(jnp.exp(draws), dims[position] // parts).reshape((-1,) + (1,) * (len(dims) - position - 1))

    gain = one(*cuts[0])
    for cut in cuts[1:]:
        gain = gain * one(*cut)
    return gain


def noise(rng, extent, deviation, limit, cuts=(), dtype=jnp.bfloat16):
    factor_of = steps_of(rng, extent, cuts, -0.22, 0.18) if cuts else 1.0
    values = jax.random.normal(rng, extent, jnp.float32) * deviation * factor_of
    return jnp.minimum(jnp.maximum(values, -limit), limit).astype(dtype)


def setup_inputs(seed: int = 0) -> dict:
    streams_of = jax.random.split(jax.random.key(seed), 7)
    weights_in = noise(streams_of[0], (2, D, FF), 1.0, 6.0, ((1, 8), (2, 4)), jnp.float32)
    weights_mix = noise(streams_of[1], (D, D), 1.0, 6.0, ((0, 8), (1, 4)), jnp.float32)
    momentum_in = draw_momentum_in(jax.random.fold_in(streams_of[6], 71), 0)
    momentum_mix = draw_momentum_mix(jax.random.fold_in(streams_of[6], 71), 0)
    grads_in = draw_grads_in(jax.random.fold_in(streams_of[6], 71), 0)
    grads_mix = draw_grads_mix(jax.random.fold_in(streams_of[6], 71), 0)
    return {"weights_in": weights_in, "weights_mix": weights_mix, "momentum_in": momentum_in, "momentum_mix": momentum_mix, "grads_in": grads_in, "grads_mix": grads_mix}


A_COEF = 3.4445
B_COEF = -4.775
C_COEF = 2.0315
MOMENTUM_DECAY = 0.95
STEP_RATE = 0.02
HIGH = lax.Precision.HIGHEST

def orthogonal(moment):
    row_total, col_total = moment.shape
    current = moment
    for iteration in range(ITERS):
        gram_sum = jnp.dot(current, current.T, precision=HIGH)
        if iteration == 0:
            scaling = 0.5 * lax.rsqrt(jnp.maximum(jnp.trace(gram_sum) / D, 1.0))
        else:
            scaling = jnp.float32(1.0)
        square = jnp.dot(gram_sum, gram_sum, precision=HIGH)
        poly_mat = scaling ** 2 * B_COEF * gram_sum + scaling ** 4 * C_COEF * square
        current = scaling * (A_COEF * current + jnp.dot(poly_mat, current, precision=HIGH))
    return current * math.sqrt(max(row_total, col_total))

def reference(weights_in, weights_mix, momentum_in, momentum_mix, grads_in, grads_mix):
    moment_in = MOMENTUM_DECAY * momentum_in + grads_in
    moment_mix = MOMENTUM_DECAY * momentum_mix + grads_mix
    step_in = jnp.stack([orthogonal(moment_in[0]), orthogonal(moment_in[1])])
    step_mix = orthogonal(moment_mix)
    return (moment_in, moment_mix, weights_in - STEP_RATE * step_in, weights_mix - STEP_RATE * step_mix, step_in, step_mix)
```

```python
import functools

import jax
import jax.numpy as jnp
from jax import lax
from jax.experimental import pallas as pl
from jax.experimental.pallas import tpu as pltpu
from jax.sharding import Mesh, PartitionSpec as P

A_COEF = 3.4445
B_COEF = -4.775
C_COEF = 2.0315
MOMENTUM_DECAY = 0.95
STEP_RATE = 0.02
GROUPS = 4
MIX_GROUP = 0
IN_GROUPS = (1, 2)
MESH = pl.DeviceIdType.MESH
LANES = 128


def halves(a):
    high = lax.reduce_precision(a, exponent_bits=8, mantissa_bits=7)
    return high.astype(jnp.bfloat16), (a - high).astype(jnp.bfloat16)


def deep(a, b, dims):
    ah, al = halves(a)
    bh, bl = halves(b)
    left = jnp.concatenate([ah, al, ah], axis=dims[0])
    right = jnp.concatenate([bh, bh, bl], axis=dims[1])
    return lax.dot_general(
        left, right, (((dims[0],), (dims[1],)), ((), ())), preferred_element_type=jnp.float32
    )


def unfold(window):
    size, _, block = window.shape
    half = size // 2

    def tile(r, c):
        ahead = (r - c) % size
        if ahead <= half:
            return window[c, ahead * block : (ahead + 1) * block]
        back = size - ahead
        return window[r, back * block : (back + 1) * block].T

    return jnp.concatenate(
        [jnp.concatenate([tile(r, c) for c in range(size)], axis=1) for r in range(size)], axis=0
    )


def split_store(high_ref, low_ref, index, value):
    high = value.astype(jnp.bfloat16)
    high_ref[index] = high
    low_ref[index] = (value - high.astype(jnp.float32)).astype(jnp.bfloat16)


def thin_store(parts, index, value):
    for part in parts:
        piece = value.astype(jnp.bfloat16)
        part[index] = piece
        value = value - piece.astype(jnp.float32)


def product(gram, pair, emit, rows_per=512, fine=False):
    high_ref, low_ref = gram
    rows_per = min(rows_per, high_ref.shape[0])

    def body(i, carry):
        rows = pl.ds(pl.multiple_of(i * rows_per, rows_per), rows_per)
        high = high_ref[rows, :]
        value = jnp.dot(high, pair[0][...], preferred_element_type=jnp.float32)
        value += jnp.dot(high, pair[1][...], preferred_element_type=jnp.float32)
        low = low_ref[rows, :]
        rest = jnp.dot(low, pair[0][...], preferred_element_type=jnp.float32)
        if fine:
            rest += jnp.dot(low, pair[1][...], preferred_element_type=jnp.float32)
            rest += jnp.dot(high, pair[2][...], preferred_element_type=jnp.float32)
        value += rest
        emit(rows, value)
        return carry

    lax.fori_loop(0, high_ref.shape[0] // rows_per, body, 0)


def poly_step(gram, v, s, pair, other, scale=None, fine=False):
    once, twice = B_COEF, C_COEF
    if scale is not None:
        once, twice = B_COEF * scale, C_COEF * scale * scale

    def first(rows, value):
        s[rows, :] = value
        thin_store(other, (rows, slice(None)), value)

    def second(rows, value):
        value = A_COEF * v[rows, :] + once * s[rows, :] + twice * value
        v[rows, :] = value
        thin_store(pair, (rows, slice(None)), value)

    product(gram, pair, first, fine=fine)
    product(gram, other, second, fine=fine)


def begin(win, position, scale, v, pair):
    size, _, block, _ = win.shape
    half = size // 2

    def put(ahead, value):
        rows = pl.ds(pl.multiple_of(lax.rem(position + ahead, size) * block, block), block)
        if scale is not None:
            value = value * scale
        v[rows, :] = value
        thin_store(pair, (rows, slice(None)), value)

    def upper(ahead, carry):
        put(ahead, win[position, ahead])
        return carry

    def lower(ahead, carry):
        put(ahead, win[lax.rem(position + ahead, size), size - ahead].T)
        return carry

    lax.fori_loop(0, half + 1, upper, 0)
    lax.fori_loop(half + 1, size, lower, 0)


class Place:
    def __init__(self):
        self.g, self.h, self.tp = lax.axis_index("g"), lax.axis_index("h"), lax.axis_index("tp")
        self.core = lax.rem(self.tp, 2)
        self.chip = self.tp // 2
        self.position = self.at(0, 0, self.core)
        self.mate = self.device(0, 0, 1 - self.core)
        self.near = self.device(1, 0, self.core)
        self.far = self.device(0, 1, self.core)

    def turns(self, near, far, core):
        return near * core + far * (1 - core), near * (1 - core) + far * core

    def at(self, near, far, core):
        turn_h, turn_chip = self.turns(near, far, core)
        return (
            lax.rem(self.h + turn_h, 2) * 4 + lax.rem(self.chip + turn_chip, 2) * 2 + core
        )

    def device(self, near, far, core):
        turn_h, turn_chip = self.turns(near, far, core)
        return (
            self.g,
            lax.rem(self.h + turn_h, 2),
            lax.rem(self.chip + turn_chip, 2) * 2 + core,
        )

    def greet(self):
        barrier = pltpu.get_barrier_semaphore()
        peers = (self.mate, self.near, self.far)
        for peer in peers:
            pl.semaphore_signal(barrier, inc=1, device_id=peer, device_id_type=MESH)
        pl.semaphore_wait(barrier, len(peers))


def gather(place, slab, win, send, recv, gram, idle=None):
    size, tall, block, _ = win.shape
    half = size // 2
    high, low = gram
    me, other = place.position, 1 - place.core
    slots = (
        place.at(1, 0, place.core),
        place.at(0, 1, place.core),
        place.at(1, 1, place.core),
        place.at(0, 0, other),
        place.at(1, 0, other),
        place.at(0, 1, other),
        place.at(1, 1, other),
    )

    def copy(kind, j, slot, dest, src=None):
        return pltpu.make_async_remote_copy(
            src_ref=win.at[slot, j] if src is None else src.at[j],
            dst_ref=win.at[slot, j],
            send_sem=send.at[kind, j],
            recv_sem=recv.at[kind, j],
            device_id=dest,
            device_id_type=MESH,
        )

    def got(kind, j):
        copy(kind, j, slots[kind], place.mate).wait_recv()

    def store(slot, j):
        tile = win[slot, j]
        at_c = pl.ds(pl.multiple_of(slot * block, block), block)
        at_r = pl.ds(pl.multiple_of(lax.rem(slot + j, size) * block, block), block)
        split_store(high, low, (at_r, at_c), tile)

        @pl.when((j > 0) & (j < half))
        def _():
            split_store(high, low, (at_c, at_r), tile.T)

    def start(j, carry):
        copy(0, j, me, place.near, slab).start()
        copy(1, j, me, place.far, slab).start()
        copy(3, j, me, place.mate, slab).start()
        return carry

    lax.fori_loop(0, tall, start, 0)

    def first(j, carry):
        win[me, j] = slab[j]
        store(me, j)
        got(3, j)
        store(slots[3], j)
        return carry

    lax.fori_loop(0, tall, first, 0)
    if idle is not None:
        idle()

    def main(j, carry):
        got(0, j)
        copy(2, j, slots[0], place.far).start()
        copy(4, j, slots[0], place.mate).start()
        got(1, j)
        copy(5, j, slots[1], place.mate).start()
        store(slots[0], j)
        store(slots[1], j)
        got(4, j)
        store(slots[4], j)
        got(5, j)
        store(slots[5], j)
        return carry

    lax.fori_loop(0, tall, main, 0)

    def last(j, carry):
        got(2, j)
        copy(6, j, slots[2], place.mate).start()
        store(slots[2], j)
        got(6, j)
        store(slots[6], j)
        return carry

    lax.fori_loop(0, tall, last, 0)

    def drain(j, carry):
        for kind in range(7):
            copy(kind, j, slots[kind], place.mate).wait_send()
        return carry

    lax.fori_loop(0, tall, drain, 0)


def next_gram_steps(gram, v, s, pair, other, scale):
    poly_step(gram, v, s, pair, other, scale, True)
    poly_step(gram, v, s, pair, other, scale, True)


def put_window(v, position, out_ref, size):
    tall, block, _ = out_ref.shape
    for ahead in range(tall):
        row = lax.rem(position + ahead, size) * block
        out_ref[ahead] = v[pl.ds(pl.multiple_of(row, block), block), :]


def gram_kernel(x_ref, out_ref, left, right, part, acc, mated, neared, farred, send, recv):
    total, wide = x_ref.shape
    tall, block, _ = out_ref.shape
    size = total // block
    place = Place()
    place.greet()

    def split(i, carry):
        rows = pl.ds(pl.multiple_of(i * block, block), block)
        value = x_ref[rows, :]
        for k in range(3):
            piece = value.astype(jnp.bfloat16)
            value = value - piece.astype(jnp.float32)
            left[rows, k * wide : (k + 1) * wide] = piece
            right[rows, (2 - k) * wide : (3 - k) * wide] = piece

            @pl.when(i < tall - 1)
            def _():
                again = pl.ds(pl.multiple_of(i * block + total, block), block)
                left[again, k * wide : (k + 1) * wide] = piece

        return carry

    lax.fori_loop(0, size, split, 0)

    def partial(ref, k, target):
        rows = pl.ds(pl.multiple_of(target * block, block), tall * block)
        cols = pl.ds(pl.multiple_of(target * block, block), block)
        value = None
        for depth in (3, 2, 1):
            term = lax.dot_general(
                left[rows, : depth * wide],
                right[cols, (3 - depth) * wide :],
                (((1,), (1,)), ((), ())),
                preferred_element_type=jnp.float32,
            )
            value = term if value is None else value + term
        ref[k] = value.reshape(tall, block, block)

    def copy(kind, src, dst, dest):
        return pltpu.make_async_remote_copy(
            src_ref=src,
            dst_ref=dst,
            send_sem=send.at[kind],
            recv_sem=recv.at[kind],
            device_id=dest,
            device_id_type=MESH,
        )

    def to_mate(k):
        return copy(k, part.at[k], mated.at[k], place.mate)

    def to_near(k):
        return copy(4 + k, acc.at[k], neared.at[k], place.near)

    to_far = copy(6, acc.at[2], farred, place.far)

    def step(k, carry):
        near, far = (3 - k) // 2, lax.rem(3 - k, 2)
        partial(part, k, place.at(near, far, 1 - place.core))
        to_mate(k).start()
        partial(acc, k, place.at(near, far, place.core))
        to_mate(k).wait_recv()
        acc[k] = acc[k] + mated[k]

        @pl.when(k < 2)
        def _():
            to_near(k).start()

        @pl.when(k == 2)
        def _():
            to_near(0).wait_recv()
            acc[2] = acc[2] + neared[0]
            to_far.start()

        return carry

    lax.fori_loop(0, 4, step, 0)
    to_near(1).wait_recv()
    acc[3] = acc[3] + neared[1]
    to_far.wait_recv()
    out_ref[...] = acc[3] + farred[...]
    for k in range(4):
        to_mate(k).wait_send()
    to_near(0).wait_send()
    to_near(1).wait_send()
    to_far.wait_send()


def first_kernel(total, slab, high, low, out_ref, scale_ref, win, v, s, send, recv, *pairs):
    size, tall, block, _ = win.shape
    place = Place()
    place.greet()
    gather(place, slab, win, send, recv, (high, low))
    row = lax.broadcasted_iota(jnp.int32, (block, block), 0)
    col = lax.broadcasted_iota(jnp.int32, (block, block), 1)
    diagonal = win[0, 0]
    for i in range(1, size):
        diagonal = diagonal + win[i, 0]
    ssq = jnp.sum(jnp.where(row == col, diagonal, 0.0))
    scale = 0.25 / jnp.maximum(ssq / total, 1.0)
    scale_ref[0] = scale
    begin(win, place.position, scale, v, pairs[:3])
    next_gram_steps((high, low), v, s, pairs[:3], pairs[3:], scale)
    put_window(v, place.position, out_ref, size)


def second_kernel(scale_ref, slab, high0, low0, out_ref, win, high1, low1, v, s, kept, send, recv, *pairs):
    size, tall, block, _ = win.shape
    total = v.shape[0]
    gram0, gram1 = (high0, low0), (high1, low1)
    pair, other = pairs[:3], pairs[3:]
    place = Place()
    position = place.position
    place.greet()
    gather(place, slab, win, send, recv, gram1)
    begin(win, position, None, v, pair)
    next_gram_steps(gram1, v, s, pair, other, None)

    def keep(rows, value):
        kept[rows, :] = v[rows, :]
        v[rows, :] = value
        thin_store(other, (rows, slice(None)), value)

    product(gram1, pair, keep)
    poly_step(gram1, v, s, other, pair)
    poly_step(gram1, v, s, other, pair)
    step = min(512, total)

    def weights(i, carry):
        rows = pl.ds(pl.multiple_of(i * step, step), step)
        row = lax.broadcasted_iota(jnp.int32, (step, block), 0) + i * step
        col = lax.broadcasted_iota(jnp.int32, (step, block), 1) + position * block
        value = (
            jnp.where(row == col, A_COEF, 0.0) + B_COEF * kept[rows, :] + C_COEF * v[rows, :]
        )
        v[rows, :] = value
        thin_store(pair, (rows, slice(None)), value)
        return carry

    lax.fori_loop(0, total // step, weights, 0)
    poly_step(gram1, v, s, pair, other)
    poly_step(gram0, v, s, pair, other, scale_ref[0])
    put_window(v, position, out_ref, size)


def last_kernel(gain_ref, slab, x_ref, out_ref, win, high, low, xh, xl, send, recv):
    block = win.shape[2]
    place = Place()
    place.greet()

    def idle():
        def split(i, carry):
            rows = pl.ds(pl.multiple_of(i * block, block), block)
            split_store(xh, xl, (rows, slice(None)), x_ref[rows, :])
            return carry

        lax.fori_loop(0, x_ref.shape[0] // block, split, 0)

    gather(place, slab, win, send, recv, (high, low), idle)

    def emit(rows, value):
        out_ref[rows, :] = value * gain_ref[0]

    product((high, low), (xh, xl), emit, 256)


def run(kernel, outs, scratch, scalars, arrays, ident):
    def spec(out):
        return pl.BlockSpec(memory_space=pltpu.SMEM if out.size == 1 else pltpu.VMEM)

    return pl.pallas_call(
        kernel,
        out_shape=outs,
        in_specs=[pl.BlockSpec(memory_space=pltpu.SMEM)] * len(scalars)
        + [pl.BlockSpec(memory_space=pltpu.VMEM)] * len(arrays),
        out_specs=jax.tree.map(spec, outs),
        scratch_shapes=scratch,
        compiler_params=pltpu.CompilerParams(
            vmem_limit_bytes=67043328, collective_id=ident, has_side_effects=True
        ),
    )(*scalars, *arrays)


def update_kernels(x, block, gain_of):
    total, wide = x.shape
    size = total // block
    tall = size // 2 + 1
    bf16, f32 = jnp.bfloat16, jnp.float32
    slab_shape = (tall, block, block)
    slab = jax.ShapeDtypeStruct(slab_shape, f32)
    whole = jax.ShapeDtypeStruct((total, total), bf16)
    full, thin = pltpu.VMEM((total, total), bf16), pltpu.VMEM((total, block), f32)
    win = pltpu.VMEM((size,) + slab_shape, f32)
    sems = [pltpu.SemaphoreType.DMA((7, tall))] * 2
    pairs = [pltpu.VMEM((total, block), bf16)] * 6
    mine = run(
        gram_kernel,
        slab,
        [
            pltpu.VMEM((total + (tall - 1) * block, 3 * wide), bf16),
            pltpu.VMEM((total, 3 * wide), bf16),
            pltpu.VMEM((4,) + slab_shape, f32),
            pltpu.VMEM((4,) + slab_shape, f32),
            pltpu.VMEM((4,) + slab_shape, f32),
            pltpu.VMEM((2,) + slab_shape, f32),
            pltpu.VMEM(slab_shape, f32),
            pltpu.SemaphoreType.DMA((7,)),
            pltpu.SemaphoreType.DMA((7,)),
        ],
        (),
        (x,),
        0,
    )
    high0, low0, mine, scale = run(
        functools.partial(first_kernel, total),
        (whole, whole, slab, jax.ShapeDtypeStruct((1,), f32)),
        [win, thin, thin] + sems + pairs,
        (),
        (mine,),
        1,
    )
    mine = run(
        second_kernel,
        slab,
        [win, full, full, thin, thin, thin] + sems + pairs,
        (scale,),
        (mine, high0, low0),
        2,
    )
    return run(
        last_kernel,
        jax.ShapeDtypeStruct((total, wide), f32),
        [win, full, full] + [pltpu.VMEM((total, wide), bf16)] * 2 + sems,
        (gain_of(jnp.sqrt(scale)),),
        (mine, x),
        3,
    )


def chain_plain(window, position, scale_sq, share):
    size, tall, block = window.shape
    total = size * block

    def product_of(gram, v):
        return deep(gram, v, (1, 0))

    def poly(gram, v):
        once = product_of(gram, v)
        return A_COEF * v + B_COEF * once + C_COEF * product_of(gram, once)

    def columns(full):
        return lax.dynamic_slice(full, (0, position * block), (total, block))

    def crop(v):
        return lax.dynamic_slice(
            jnp.concatenate([v, v], axis=0), (position * block, 0), (tall, block)
        )

    gram0 = unfold(window) * scale_sq
    gram1 = unfold(share(crop(poly(gram0, poly(gram0, columns(gram0))))))
    v2 = poly(gram1, poly(gram1, columns(gram1)))
    square = poly(gram1, poly(gram1, product_of(gram1, v2)))
    w = A_COEF * columns(jnp.eye(total, dtype=jnp.float32)) + B_COEF * v2 + C_COEF * square
    return share(crop(poly(gram0, poly(gram1, w))))


def apply_plain(window, x, gain):
    return deep(unfold(window), x, (1, 0)) * gain


def update_plain(x, block, gain_of, team):
    total = x.shape[0]
    size = total // block
    window = (size // 2 + 1) * block

    def share(mine):
        return lax.all_gather(mine, team, axis=0, tiled=False)

    twice = jnp.concatenate([x, x[: window - block]], axis=0)
    partial = jnp.stack(
        [
            lax.dot_general(
                twice[i * block : i * block + window],
                x[i * block : (i + 1) * block],
                (((1,), (1,)), ((), ())),
                precision=lax.Precision.HIGHEST,
            )
            for i in range(size)
        ]
    )
    gram_window = share(lax.psum_scatter(partial, team, scatter_dimension=0, tiled=False))
    corner = jnp.eye(block, dtype=jnp.float32)
    ssq = jnp.sum(gram_window[:, :block, :] * corner)
    scaling = 0.5 * lax.rsqrt(jnp.maximum(ssq / total, 1.0))
    w_window = chain_plain(gram_window, lax.axis_index(team), scaling**2, share)
    return apply_plain(w_window, x, gain_of(scaling))


def solution(mesh):
    n_fs, n_tp = mesh.shape["fs"], mesh.shape["tp"]
    per = n_fs // GROUPS
    size = per * n_tp
    grid = Mesh(mesh.devices.reshape(GROUPS, per, n_tp), ("g", "h", "tp"))
    fs = ("g", "h")
    team = ("h", "tp")

    def exchange(select, shape, pairs_ok, place):
        me = lax.axis_index(fs)
        held = jnp.zeros((n_fs,) + shape, jnp.float32)
        for shift in range(n_fs):
            dest = (me + shift) % n_fs
            value = select(dest)
            if shift:
                pairs = [(f, (f + shift) % n_fs) for f in range(n_fs)]
                pairs = [p for p in pairs if pairs_ok(*p)]
                value = lax.ppermute(value, fs, pairs)
            source = (me - shift + n_fs) % n_fs
            held = lax.dynamic_update_slice(held, value[None], (source, 0, 0))
        return held

    def local(weights_in, weights_mix, momentum_in, momentum_mix, grads_in, grads_mix):
        moment_in = MOMENTUM_DECAY * momentum_in + grads_in
        moment_mix = MOMENTUM_DECAY * momentum_mix + grads_mix
        rows, cols_in = moment_in.shape[1:]
        cols_mix = moment_mix.shape[1]
        wide, narrow = cols_in // per, cols_mix // per
        total = rows * n_fs
        block = total // size
        group = lax.axis_index("g")

        def pick_in(dest):
            which = jnp.clip(dest // per - IN_GROUPS[0], 0, 1)
            return lax.dynamic_slice(moment_in, (which, 0, (dest % per) * wide), (1, rows, wide))[0]

        def pick_mix(dest):
            return lax.dynamic_slice(moment_mix, (0, (dest % per) * narrow), (rows, narrow))

        got_in = exchange(pick_in, (rows, wide), lambda f, d: d // per in IN_GROUPS, None)
        got_mix = exchange(pick_mix, (rows, narrow), lambda f, d: d // per == MIX_GROUP, None)
        kernels = block % LANES == 0 and (per, n_tp) == (2, 4)
        x = jnp.where(
            group == MIX_GROUP, jnp.pad(got_mix, ((0, 0), (0, 0), (0, wide - narrow))), got_in
        ).reshape(total, wide)
        if kernels:
            x = jnp.pad(x, ((0, 0), (0, -wide % LANES)))

        columns = jnp.where(group == MIX_GROUP, cols_mix, cols_in) * n_tp
        root = jnp.sqrt(jnp.maximum(columns, total).astype(jnp.float32))

        def gain_of(scaling):
            return root * scaling

        if kernels:
            update = update_kernels(x, block, gain_of)
        else:
            update = update_plain(x, block, gain_of, team)
        update = update.reshape((n_fs, rows) + update.shape[1:])

        def out_in(dest):
            return lax.dynamic_slice(update, (dest, 0, 0), (1, rows, wide))[0]

        def out_mix(dest):
            return lax.dynamic_slice(update, (dest, 0, 0), (1, rows, narrow))[0]

        back_in = exchange(out_in, (rows, wide), lambda f, d: f // per in IN_GROUPS, None)
        back_mix = exchange(out_mix, (rows, narrow), lambda f, d: f // per == MIX_GROUP, None)
        step_in = jnp.stack(
            [
                jnp.concatenate([back_in[g * per + h] for h in range(per)], axis=1)
                for g in IN_GROUPS
            ]
        )
        step_mix = jnp.concatenate(
            [back_mix[MIX_GROUP * per + h] for h in range(per)], axis=1
        )
        return (
            moment_in,
            moment_mix,
            weights_in - STEP_RATE * step_in,
            weights_mix - STEP_RATE * step_mix,
            step_in,
            step_mix,
        )

    big = P(None, fs, "tp")
    small = P(fs, "tp")
    specs = (big, small, big, small, big, small)
    return jax.shard_map(local, mesh=grid, in_specs=specs, out_specs=specs, check_vma=False)
```

```python
import functools

import jax
import jax.numpy as jnp
from jax import lax
from jax.experimental import pallas as pl
from jax.experimental.pallas import tpu as pltpu
from jax.sharding import Mesh, PartitionSpec as P

A_COEF = 3.4445
B_COEF = -4.775
C_COEF = 2.0315
MOMENTUM_DECAY = 0.95
STEP_RATE = 0.02
GROUPS = 4
MIX_GROUP = 0
IN_GROUPS = (1, 2)
MESH = pl.DeviceIdType.MESH
LANES = 128


def halves(a):
    high = lax.reduce_precision(a, exponent_bits=8, mantissa_bits=7)
    return high.astype(jnp.bfloat16), (a - high).astype(jnp.bfloat16)


def deep(a, b, dims):
    ah, al = halves(a)
    bh, bl = halves(b)
    left = jnp.concatenate([ah, al, ah], axis=dims[0])
    right = jnp.concatenate([bh, bh, bl], axis=dims[1])
    return lax.dot_general(
        left, right, (((dims[0],), (dims[1],)), ((), ())), preferred_element_type=jnp.float32
    )


def unfold(window):
    size, _, block = window.shape
    half = size // 2

    def tile(r, c):
        ahead = (r - c) % size
        if ahead <= half:
            return window[c, ahead * block : (ahead + 1) * block]
        back = size - ahead
        return window[r, back * block : (back + 1) * block].T

    return jnp.concatenate(
        [jnp.concatenate([tile(r, c) for c in range(size)], axis=1) for r in range(size)], axis=0
    )


def split_store(high_ref, low_ref, index, value):
    high = value.astype(jnp.bfloat16)
    high_ref[index] = high
    low_ref[index] = (value - high.astype(jnp.float32)).astype(jnp.bfloat16)


def thin_store(parts, index, value):
    for part in parts:
        piece = value.astype(jnp.bfloat16)
        part[index] = piece
        value = value - piece.astype(jnp.float32)


def product(gram, pair, emit, rows_per=512, fine=False, order=None, count=None):
    high_ref, low_ref = gram
    rows_per = min(rows_per, high_ref.shape[0])

    def body(i, carry):
        at = i if order is None else order(i)
        rows = pl.ds(pl.multiple_of(at * rows_per, rows_per), rows_per)
        high = high_ref[rows, :]
        value = jnp.dot(high, pair[0][...], preferred_element_type=jnp.float32)
        value += jnp.dot(high, pair[1][...], preferred_element_type=jnp.float32)
        low = low_ref[rows, :]
        rest = jnp.dot(low, pair[0][...], preferred_element_type=jnp.float32)
        if fine:
            rest += jnp.dot(low, pair[1][...], preferred_element_type=jnp.float32)
            rest += jnp.dot(high, pair[2][...], preferred_element_type=jnp.float32)
        value += rest
        if order is None:
            emit(rows, value)
        else:
            emit(i, at, rows, value)
        return carry

    lax.fori_loop(0, count or high_ref.shape[0] // rows_per, body, 0)


def poly_step(gram, v, s, pair, other, scale=None, fine=False, ends=None):
    once, twice = B_COEF, C_COEF
    if scale is not None:
        once, twice = B_COEF * scale, C_COEF * scale * scale

    pieces = 3 if fine else 2

    def first(rows, value):
        s[rows, :] = value
        thin_store(other[:pieces], (rows, slice(None)), value)

    def second(rows, value):
        value = A_COEF * v[rows, :] + once * s[rows, :] + twice * value
        v[rows, :] = value
        thin_store(pair[:pieces], (rows, slice(None)), value)

    product(gram, pair, first, fine=fine)
    if ends is None:
        product(gram, other, second, fine=fine)
        return
    position, out_ref = ends
    tall, block, _ = out_ref.shape
    size = v.shape[0] // block

    def window(i, at, rows, value):
        out_ref[i] = A_COEF * v[rows, :] + once * s[rows, :] + twice * value

    product(gram, other, window, block, fine, lambda i: lax.rem(position + i, size), tall)


def begin(win, position, scale, v, pair):
    size, _, block, _ = win.shape
    half = size // 2

    def put(ahead, value):
        rows = pl.ds(pl.multiple_of(lax.rem(position + ahead, size) * block, block), block)
        if scale is not None:
            value = value * scale
        v[rows, :] = value
        thin_store(pair, (rows, slice(None)), value)

    def upper(ahead, carry):
        put(ahead, win[position, ahead])
        return carry

    def lower(ahead, carry):
        put(ahead, win[lax.rem(position + ahead, size), size - ahead].T)
        return carry

    lax.fori_loop(0, half + 1, upper, 0)
    lax.fori_loop(half + 1, size, lower, 0)


class Place:
    def __init__(self):
        self.g, self.h, self.tp = lax.axis_index("g"), lax.axis_index("h"), lax.axis_index("tp")
        self.core = lax.rem(self.tp, 2)
        self.chip = self.tp // 2
        self.position = self.at(0, 0, self.core)
        self.holder = self.g * 2 + self.h
        self.mate = self.device(0, 0, 1 - self.core)
        self.near = self.device(1, 0, self.core)
        self.far = self.device(0, 1, self.core)

    def turns(self, near, far, core):
        return near * core + far * (1 - core), near * (1 - core) + far * core

    def at(self, near, far, core):
        turn_h, turn_chip = self.turns(near, far, core)
        return (
            lax.rem(self.h + turn_h, 2) * 4 + lax.rem(self.chip + turn_chip, 2) * 2 + core
        )

    def device(self, near, far, core):
        turn_h, turn_chip = self.turns(near, far, core)
        return (
            self.g,
            lax.rem(self.h + turn_h, 2),
            lax.rem(self.chip + turn_chip, 2) * 2 + core,
        )

    def row(self, index):
        return (index // 2, lax.rem(index, 2), self.tp)

    def greet(self, n_rows=None):
        barrier = pltpu.get_barrier_semaphore()

        def signal(peer):
            pl.semaphore_signal(barrier, inc=1, device_id=peer, device_id_type=MESH)

        if n_rows is None:
            peers = (self.mate, self.near, self.far)
        else:
            beside = (self.g, self.h, lax.rem(self.tp + 2, 4))
            peers = (self.mate, beside) + tuple(
                self.row(lax.rem(self.holder + i, n_rows)) for i in range(1, n_rows)
            )
        for peer in peers:
            signal(peer)
        pl.semaphore_wait(barrier, len(peers))

    def is_at(self, group, half):
        return (self.g == group) & (self.h == half)


def gather(place, slab, win, send, recv, gram, idle=None):
    size, tall, block, _ = win.shape
    half = size // 2
    high, low = gram
    me, other = place.position, 1 - place.core
    slots = (
        place.at(1, 0, place.core),
        place.at(0, 1, place.core),
        place.at(1, 1, place.core),
        place.at(0, 0, other),
        place.at(1, 0, other),
        place.at(0, 1, other),
        place.at(1, 1, other),
    )

    def copy(kind, j, slot, dest, src=None):
        return pltpu.make_async_remote_copy(
            src_ref=win.at[slot, j] if src is None else src.at[j],
            dst_ref=win.at[slot, j],
            send_sem=send.at[kind, j],
            recv_sem=recv.at[kind, j],
            device_id=dest,
            device_id_type=MESH,
        )

    def got(kind, j):
        copy(kind, j, slots[kind], place.mate).wait_recv()

    def store(slot, j):
        tile = win[slot, j]
        at_c = pl.ds(pl.multiple_of(slot * block, block), block)
        at_r = pl.ds(pl.multiple_of(lax.rem(slot + j, size) * block, block), block)
        split_store(high, low, (at_r, at_c), tile)

        @pl.when((j > 0) & (j < half))
        def _():
            split_store(high, low, (at_c, at_r), tile.T)

    def start(j, carry):
        copy(0, j, me, place.near, slab).start()
        copy(1, j, me, place.far, slab).start()
        copy(3, j, me, place.mate, slab).start()
        return carry

    lax.fori_loop(0, tall, start, 0)

    def first(j, carry):
        win[me, j] = slab[j]
        store(me, j)
        got(3, j)
        store(slots[3], j)
        return carry

    lax.fori_loop(0, tall, first, 0)
    if idle is not None:
        idle()

    def main(j, carry):
        got(0, j)
        copy(2, j, slots[0], place.far).start()
        copy(4, j, slots[0], place.mate).start()
        got(1, j)
        copy(5, j, slots[1], place.mate).start()
        store(slots[0], j)
        store(slots[1], j)
        got(4, j)
        store(slots[4], j)
        got(5, j)
        store(slots[5], j)
        return carry

    lax.fori_loop(0, tall, main, 0)

    def last(j, carry):
        got(2, j)
        copy(6, j, slots[2], place.mate).start()
        store(slots[2], j)
        got(6, j)
        store(slots[6], j)
        return carry

    lax.fori_loop(0, tall, last, 0)

    def drain(j, carry):
        for kind in range(7):
            copy(kind, j, slots[kind], place.mate).wait_send()
        return carry

    lax.fori_loop(0, tall, drain, 0)


def lead_of(cols):
    return -(-cols // (2 * LANES)) * LANES


def holders(refs):
    inward, mix = refs
    found = []
    for group in IN_GROUPS + (MIX_GROUP,):
        ref = mix if group == MIX_GROUP else inward.at[group - IN_GROUPS[0]]
        cols = ref.shape[-1]
        for half in range(2):
            start = half * lead_of(cols)
            width = lead_of(cols) if half == 0 else cols - start
            found.append((group, half, slice(start, start + width), ref))
    return found


def gram_kernel(
    in_ref, mix_ref, x_ref, out_ref, left, right, acc, mated, neared, farred, *sems
):
    send, recv, row_send, row_recv = sems
    total, wide = x_ref.shape
    tall, block, _ = out_ref.shape
    size = total // block
    place = Place()
    mine = pl.ds(pl.multiple_of(place.holder * block, block), block)
    parts = holders((in_ref, mix_ref))
    place.greet(size)

    def give(k, source):
        group, half, cols, ref = parts[k]
        width = cols.stop - cols.start
        rows = pl.ds(pl.multiple_of(source * block, block), block)
        return pltpu.make_async_remote_copy(
            src_ref=ref.at[:, cols],
            dst_ref=x_ref.at[rows, :width],
            send_sem=row_send.at[k],
            recv_sem=row_recv.at[source],
            device_id=(group, half, place.tp),
            device_id_type=MESH,
        )

    def send_rows(ks):
        for k in ks:
            group, half, _, _ = parts[k]

            @pl.when(jnp.logical_not(place.is_at(group, half)))
            def _():
                give(k, place.holder).start()

    @pl.when(place.g < GROUPS - 1)
    def _():
        send_rows(range(len(parts)))

    @pl.when(place.g == GROUPS - 1)
    def _():
        send_rows((2, 3, 0, 1, 4, 5))

    for group, half, cols, ref in parts:
        width = cols.stop - cols.start

        @pl.when(place.is_at(group, half))
        def _():
            x_ref[mine, :width] = ref[:, cols]
            if width < wide:
                x_ref[:, width:] = jnp.zeros((total, wide - width), jnp.float32)

    @pl.when(place.g == GROUPS - 1)
    def _():
        x_ref[...] = jnp.zeros_like(x_ref)

    def split(i, carry):
        for k, (group, half, _, _) in enumerate(parts):
            @pl.when(place.is_at(group, half) & (i != place.holder))
            def _():
                give(k, i).wait_recv()

        rows = pl.ds(pl.multiple_of(i * block, block), block)
        value = x_ref[rows, :]
        for k in range(3):
            piece = value.astype(jnp.bfloat16)
            value = value - piece.astype(jnp.float32)
            left[rows, k * wide : (k + 1) * wide] = piece
            right[rows, (2 - k) * wide : (3 - k) * wide] = piece

            @pl.when(i < tall - 1)
            def _():
                again = pl.ds(pl.multiple_of(i * block + total, block), block)
                left[again, k * wide : (k + 1) * wide] = piece

        return carry

    lax.fori_loop(0, size, split, 0)

    def partial(i, target):
        rows = pl.ds(pl.multiple_of(target * block, block), tall * block)
        cols = pl.ds(pl.multiple_of(target * block, block), block)
        value = None
        for depth in (3, 2, 1):
            term = lax.dot_general(
                left[rows, : depth * wide],
                right[cols, (3 - depth) * wide :],
                (((1,), (1,)), ((), ())),
                preferred_element_type=jnp.float32,
            )
            value = term if value is None else value + term
        acc[i] = value.reshape(tall, block, block)

    def copy(kind, src, dst, dest):
        return pltpu.make_async_remote_copy(
            src_ref=src,
            dst_ref=dst,
            send_sem=send.at[kind],
            recv_sem=recv.at[kind],
            device_id=dest,
            device_id_type=MESH,
        )

    def to_mate(k):
        return copy(k, acc.at[2 * k], mated.at[k], place.mate)

    def to_near(k):
        return copy(4 + k, acc.at[2 * k + 1], neared.at[k], place.near)

    to_far = copy(6, acc.at[5], farred, place.far)

    def step(i, carry):
        k, own = i // 2, lax.rem(i, 2)
        core = place.core * own + (1 - place.core) * (1 - own)
        partial(i, place.at((3 - k) // 2, lax.rem(3 - k, 2), core))

        @pl.when(own == 0)
        def _():
            to_mate(k).start()

        @pl.when(own == 1)
        def _():
            to_mate(k).wait_recv()
            acc[i] = acc[i] + mated[k]

        @pl.when((own == 1) & (k < 2))
        def _():
            to_near(k).start()

        @pl.when((own == 1) & (k == 2))
        def _():
            to_near(0).wait_recv()
            acc[i] = acc[i] + neared[0]
            to_far.start()

        return carry

    lax.fori_loop(0, 8, step, 0)
    to_near(1).wait_recv()
    acc[7] = acc[7] + neared[1]
    to_far.wait_recv()
    out_ref[...] = acc[7] + farred[...]
    for k in range(4):
        to_mate(k).wait_send()
    to_near(0).wait_send()
    to_near(1).wait_send()
    to_far.wait_send()
    for k, (group, half, _, _) in enumerate(parts):
        @pl.when(jnp.logical_not(place.is_at(group, half)))
        def _():
            give(k, place.holder).wait_send()


def first_kernel(total, slab, high, low, out_ref, scale_ref, win, v, s, send, recv, *pairs):
    size, tall, block, _ = win.shape
    place = Place()
    place.greet()
    gather(place, slab, win, send, recv, (high, low))
    row = lax.broadcasted_iota(jnp.int32, (block, block), 0)
    col = lax.broadcasted_iota(jnp.int32, (block, block), 1)
    diagonal = win[0, 0]
    for i in range(1, size):
        diagonal = diagonal + win[i, 0]
    ssq = jnp.sum(jnp.where(row == col, diagonal, 0.0))
    scale = 0.25 / jnp.maximum(ssq / total, 1.0)
    scale_ref[0] = scale
    begin(win, place.position, scale, v, pairs[:3])
    poly_step((high, low), v, s, pairs[:3], pairs[3:], scale, True)
    poly_step((high, low), v, s, pairs[:3], pairs[3:], scale, True, (place.position, out_ref))


def second_kernel(scale_ref, slab, high0, low0, out_ref, win, high1, low1, v, s, kept, send, recv, *pairs):
    size, tall, block, _ = win.shape
    total = v.shape[0]
    gram0, gram1 = (high0, low0), (high1, low1)
    pair, other = pairs[:3], pairs[3:]
    place = Place()
    position = place.position
    place.greet()
    gather(place, slab, win, send, recv, gram1)
    begin(win, position, None, v, pair)

    def finely(i, carry):
        poly_step(gram1, v, s, pair, other, None, True)
        return carry

    lax.fori_loop(0, 2, finely, 0)

    def keep(rows, value):
        kept[rows, :] = v[rows, :]
        v[rows, :] = value
        thin_store(other[:2], (rows, slice(None)), value)

    product(gram1, pair, keep)

    def squarely(i, carry):
        poly_step(gram1, v, s, other, pair)
        return carry

    lax.fori_loop(0, 2, squarely, 0)
    step = min(512, total)

    def weights(i, carry):
        rows = pl.ds(pl.multiple_of(i * step, step), step)
        row = lax.broadcasted_iota(jnp.int32, (step, block), 0) + i * step
        col = lax.broadcasted_iota(jnp.int32, (step, block), 1) + position * block
        value = (
            jnp.where(row == col, A_COEF, 0.0) + B_COEF * kept[rows, :] + C_COEF * v[rows, :]
        )
        v[rows, :] = value
        thin_store(pair[:2], (rows, slice(None)), value)
        return carry

    lax.fori_loop(0, total // step, weights, 0)
    poly_step(gram1, v, s, pair, other)
    poly_step(gram0, v, s, pair, other, scale_ref[0], ends=(position, out_ref))


def last_kernel(gain_ref, slab, x_ref, in_ref, mix_ref, win, high, low, xh, xl, update, *sems):
    send, recv, row_send, row_recv = sems
    size, _, block, _ = win.shape
    place = Place()
    parts = holders((in_ref, mix_ref))
    place.greet(size)

    def idle():
        def split(i, carry):
            rows = pl.ds(pl.multiple_of(i * block, block), block)
            split_store(xh, xl, (rows, slice(None)), x_ref[rows, :])
            return carry

        lax.fori_loop(0, size, split, 0)

    gather(place, slab, win, send, recv, (high, low), idle)

    def give(k, dest):
        _, _, cols, ref = parts[k]
        rows = pl.ds(pl.multiple_of(dest * block, block), block)
        return pltpu.make_async_remote_copy(
            src_ref=update.at[rows, : cols.stop - cols.start],
            dst_ref=ref.at[:, cols],
            send_sem=row_send.at[dest],
            recv_sem=row_recv.at[k],
            device_id=place.row(dest),
            device_id_type=MESH,
        )

    def order(i):
        k = i // 2
        away = (k + 2) * (1 - k // 2) + (3 - k) * (k // 2)
        return lax.rem(place.g + away, GROUPS) * 2 + lax.rem(i, 2)

    def emit(i, at, rows, value):
        update[rows, :] = value * gain_ref[0]
        for k, (group, half, cols, ref) in enumerate(parts):
            @pl.when(place.is_at(group, half) & (at != place.holder))
            def _():
                give(k, at).start()

            @pl.when(place.is_at(group, half) & (at == place.holder))
            def _():
                ref[:, cols] = update[rows, : cols.stop - cols.start]

    product((high, low), (xh, xl), emit, block, order=order)
    for k, (group, half, _, _) in enumerate(parts):
        @pl.when(jnp.logical_not(place.is_at(group, half)))
        def _():
            give(k, place.holder).wait_recv()

        def drain(i, carry):
            @pl.when(i != place.holder)
            def _():
                give(k, i).wait_send()

            return carry

        @pl.when(place.is_at(group, half))
        def _():
            lax.fori_loop(0, size, drain, 0)


def run(kernel, outs, scratch, scalars, arrays, ident):
    def spec(out):
        return pl.BlockSpec(memory_space=pltpu.SMEM if out.size == 1 else pltpu.VMEM)

    return pl.pallas_call(
        kernel,
        out_shape=outs,
        in_specs=[pl.BlockSpec(memory_space=pltpu.SMEM)] * len(scalars)
        + [pl.BlockSpec(memory_space=pltpu.VMEM)] * len(arrays),
        out_specs=jax.tree.map(spec, outs),
        scratch_shapes=scratch,
        compiler_params=pltpu.CompilerParams(
            vmem_limit_bytes=67043328, collective_id=ident, has_side_effects=True
        ),
    )(*scalars, *arrays)


def update_kernels(moment_in, moment_mix, total, block, gain_of):
    wide = max(lead_of(moment_in.shape[-1]), lead_of(moment_mix.shape[-1]))
    size = total // block
    tall = size // 2 + 1
    bf16, f32 = jnp.bfloat16, jnp.float32
    slab_shape = (tall, block, block)
    slab = jax.ShapeDtypeStruct(slab_shape, f32)
    whole = jax.ShapeDtypeStruct((total, total), bf16)
    full, thin = pltpu.VMEM((total, total), bf16), pltpu.VMEM((total, block), f32)
    win = pltpu.VMEM((size,) + slab_shape, f32)
    dma = pltpu.SemaphoreType.DMA
    sems = [dma((7, tall))] * 2
    pairs = [pltpu.VMEM((total, block), bf16)] * 6
    x, mine = run(
        gram_kernel,
        (jax.ShapeDtypeStruct((total, wide), f32), slab),
        [
            pltpu.VMEM((total + (tall - 1) * block, 3 * wide), bf16),
            pltpu.VMEM((total, 3 * wide), bf16),
            pltpu.VMEM((8,) + slab_shape, f32),
            pltpu.VMEM((4,) + slab_shape, f32),
            pltpu.VMEM((2,) + slab_shape, f32),
            pltpu.VMEM(slab_shape, f32),
            dma((7,)),
            dma((7,)),
            dma((6,)),
            dma((size,)),
        ],
        (),
        (moment_in, moment_mix),
        0,
    )
    high0, low0, mine, scale = run(
        functools.partial(first_kernel, total),
        (whole, whole, slab, jax.ShapeDtypeStruct((1,), f32)),
        [win, thin, thin] + sems + pairs,
        (),
        (mine,),
        1,
    )
    mine = run(
        second_kernel,
        slab,
        [win, full, full, thin, thin, thin] + sems + pairs,
        (scale,),
        (mine, high0, low0),
        2,
    )
    return run(
        last_kernel,
        (
            jax.ShapeDtypeStruct(moment_in.shape, f32),
            jax.ShapeDtypeStruct(moment_mix.shape, f32),
        ),
        [win, full, full]
        + [pltpu.VMEM((total, wide), bf16)] * 2
        + [pltpu.VMEM((total, wide), f32)]
        + sems
        + [dma((size,)), dma((6,))],
        (gain_of(jnp.sqrt(scale)),),
        (mine, x),
        3,
    )


def chain_plain(window, position, scale_sq, share):
    size, tall, block = window.shape
    total = size * block

    def product_of(gram, v):
        return deep(gram, v, (1, 0))

    def poly(gram, v):
        once = product_of(gram, v)
        return A_COEF * v + B_COEF * once + C_COEF * product_of(gram, once)

    def columns(full):
        return lax.dynamic_slice(full, (0, position * block), (total, block))

    def crop(v):
        return lax.dynamic_slice(
            jnp.concatenate([v, v], axis=0), (position * block, 0), (tall, block)
        )

    gram0 = unfold(window) * scale_sq
    gram1 = unfold(share(crop(poly(gram0, poly(gram0, columns(gram0))))))
    v2 = poly(gram1, poly(gram1, columns(gram1)))
    square = poly(gram1, poly(gram1, product_of(gram1, v2)))
    w = A_COEF * columns(jnp.eye(total, dtype=jnp.float32)) + B_COEF * v2 + C_COEF * square
    return share(crop(poly(gram0, poly(gram1, w))))


def apply_plain(window, x, gain):
    return deep(unfold(window), x, (1, 0)) * gain


def update_plain(x, block, gain_of, team):
    total = x.shape[0]
    size = total // block
    window = (size // 2 + 1) * block

    def share(mine):
        return lax.all_gather(mine, team, axis=0, tiled=False)

    twice = jnp.concatenate([x, x[: window - block]], axis=0)
    partial = jnp.stack(
        [
            lax.dot_general(
                twice[i * block : i * block + window],
                x[i * block : (i + 1) * block],
                (((1,), (1,)), ((), ())),
                precision=lax.Precision.HIGHEST,
            )
            for i in range(size)
        ]
    )
    gram_window = share(lax.psum_scatter(partial, team, scatter_dimension=0, tiled=False))
    corner = jnp.eye(block, dtype=jnp.float32)
    ssq = jnp.sum(gram_window[:, :block, :] * corner)
    scaling = 0.5 * lax.rsqrt(jnp.maximum(ssq / total, 1.0))
    w_window = chain_plain(gram_window, lax.axis_index(team), scaling**2, share)
    return apply_plain(w_window, x, gain_of(scaling))


def solution(mesh):
    n_fs, n_tp = mesh.shape["fs"], mesh.shape["tp"]
    per = n_fs // GROUPS
    size = per * n_tp
    grid = Mesh(mesh.devices.reshape(GROUPS, per, n_tp), ("g", "h", "tp"))
    fs = ("g", "h")
    team = ("h", "tp")

    def exchange(select, shape, pairs_ok, place):
        me = lax.axis_index(fs)
        held = jnp.zeros((n_fs,) + shape, jnp.float32)
        for shift in range(n_fs):
            dest = (me + shift) % n_fs
            value = select(dest)
            if shift:
                pairs = [(f, (f + shift) % n_fs) for f in range(n_fs)]
                pairs = [p for p in pairs if pairs_ok(*p)]
                value = lax.ppermute(value, fs, pairs)
            source = (me - shift + n_fs) % n_fs
            held = lax.dynamic_update_slice(held, value[None], (source, 0, 0))
        return held

    def local(weights_in, weights_mix, momentum_in, momentum_mix, grads_in, grads_mix):
        moment_in = MOMENTUM_DECAY * momentum_in + grads_in
        moment_mix = MOMENTUM_DECAY * momentum_mix + grads_mix
        rows, cols_in = moment_in.shape[1:]
        cols_mix = moment_mix.shape[1]
        wide, narrow = cols_in // per, cols_mix // per
        total = rows * n_fs
        block = total // size
        group = lax.axis_index("g")
        columns = jnp.where(group == MIX_GROUP, cols_mix, cols_in) * n_tp
        root = jnp.sqrt(jnp.maximum(columns, total).astype(jnp.float32))

        def gain_of(scaling):
            return root * scaling

        def results(step_in, step_mix):
            return (
                moment_in,
                moment_mix,
                weights_in - STEP_RATE * step_in,
                weights_mix - STEP_RATE * step_mix,
                step_in,
                step_mix,
            )

        lanes = all(n % LANES == 0 for n in (block, cols_in, cols_mix))
        if lanes and rows == block and (per, n_tp) == (2, 4):
            return results(*update_kernels(moment_in, moment_mix, total, block, gain_of))

        def pick_in(dest):
            which = jnp.clip(dest // per - IN_GROUPS[0], 0, 1)
            return lax.dynamic_slice(moment_in, (which, 0, (dest % per) * wide), (1, rows, wide))[0]

        def pick_mix(dest):
            return lax.dynamic_slice(moment_mix, (0, (dest % per) * narrow), (rows, narrow))

        got_in = exchange(pick_in, (rows, wide), lambda f, d: d // per in IN_GROUPS, None)
        got_mix = exchange(pick_mix, (rows, narrow), lambda f, d: d // per == MIX_GROUP, None)
        x = jnp.where(
            group == MIX_GROUP, jnp.pad(got_mix, ((0, 0), (0, 0), (0, wide - narrow))), got_in
        ).reshape(total, wide)

        update = update_plain(x, block, gain_of, team)
        update = update.reshape((n_fs, rows) + update.shape[1:])

        def out_in(dest):
            return lax.dynamic_slice(update, (dest, 0, 0), (1, rows, wide))[0]

        def out_mix(dest):
            return lax.dynamic_slice(update, (dest, 0, 0), (1, rows, narrow))[0]

        back_in = exchange(out_in, (rows, wide), lambda f, d: f // per in IN_GROUPS, None)
        back_mix = exchange(out_mix, (rows, narrow), lambda f, d: f // per == MIX_GROUP, None)
        step_in = jnp.stack(
            [
                jnp.concatenate([back_in[g * per + h] for h in range(per)], axis=1)
                for g in IN_GROUPS
            ]
        )
        step_mix = jnp.concatenate(
            [back_mix[MIX_GROUP * per + h] for h in range(per)], axis=1
        )
        return results(step_in, step_mix)

    big = P(None, fs, "tp")
    small = P(fs, "tp")
    specs = (big, small, big, small, big, small)
    return jax.shard_map(local, mesh=grid, in_specs=specs, out_specs=specs, check_vma=False)
```
